128 devices in a mesh: ep: 16 (over z, x), tp: 8 (over y, core).
Axes of the slice: x: 4, y: 4, z: 4, core: 2. Of those that a mesh axis runs over, the one named last changes fastest.
Arguments:
- mixer_in: bfloat16 [16384, 2048], P(('ep', 'tp')), may hold values from -6 to 6
- expert_in: bfloat16 [65536, 2048], P(('ep', 'tp')), may hold values from -6 to 6
- mixer_gain: float32 [2048], replicated, may hold values from 0.1 to 1.9
- query_weight: bfloat16 [2048, 1024], replicated, may hold values from -0.125 to 0.125
- key_weight: bfloat16 [2048, 128], replicated, may hold values from -0.125 to 0.125
- value_weight: bfloat16 [2048, 128], replicated, may hold values from -0.125 to 0.125
- query_gain: float32 [64], replicated, may hold values from 0.4 to 6
- key_gain: float32 [64], replicated, may hold values from 0.4 to 6
- output_weight: bfloat16 [1024, 2048], replicated, may hold values from -0.1875 to 0.1875
- expert_gain: float32 [2048], replicated, may hold values from 0.1 to 1.9
- routes: int32 [65536, 2], P(('ep', 'tp')), may hold values from 0 to 31, all different within a row; in each aligned block of 512 rows (0 to 511, 512 to 1023, ...) at most 64 rows name the same one
- route_weight: float32 [65536, 2], P(('ep', 'tp')), may hold values from 0.2 to 1.5
- gate_weight: bfloat16 [32, 2048, 512], P('ep'), may hold values from -0.125 to 0.125
- up_weight: bfloat16 [32, 2048, 512], P('ep'), may hold values from -0.125 to 0.125
- down_weight: bfloat16 [32, 512, 2048], P('ep'), may hold values from -0.25 to 0.25
Outputs:
- mixer_out: bfloat16 [16384, 2048], P(('ep', 'tp'))
- expert_out: bfloat16 [65536, 2048], P(('ep', 'tp'))
The draws below stay inside these ranges and needn't reach their ends.
Inputs may be any that keep to these rules, and one draw needn't show every extreme that they name: `routes`: each row names 2 different experts; among the rows of one device no expert is named more than 64 times, a bound that some block reaches.
All inputs are finite; a program needn't handle non-finite values.
Results may differ from the reference program's by a relative error of at most 0.0085.
The reference program's roundings to bfloat16 on the way count: a program that leaves them out, or rounds other values in their place, can miss the bound.
Values may be sent and summed in bfloat16 or wider, within the bound.
No kernel may reach another device: no remote copies, remote signals or barrier semaphores. Data moves between devices by JAX's collectives and lax.ppermute only.
A program may use at most 384 MiB of HBM per device.

```python
import math
import jax
import jax.numpy as jnp
import numpy as np
from jax import lax

D = 2048
HEAD = 64
QHEADS = 16
KVHEADS = 2
GRID = 64
FF = 512
TOPK = 2
EXP_TOK = 512
TOKENS = 16384
EXP_TOKENS = 65536
EXPERTS = 32
CAP = 64
N_EP = 16
N_TP = 8


def gain_values(key):
    return 1.0 + 0.18 * jax.random.truncated_normal(key, -3.0, 3.0, (HEAD,), jnp.float32)


def draw_query_gain(key, part):
    return gain_values(jax.random.fold_in(key, 11))


def draw_key_gain(key, part):
    return gain_values(jax.random.fold_in(key, 23))


def shard_levels(rng, shape, pieces, smallest, largest):
    level = 1.0
    for dim, shards_of in pieces:
        draws = jax.random.uniform(jax.random.fold_in(jax.random.fold_in(rng, 6), dim), (shards_of,), jnp.float32, smallest / len(pieces), largest / len(pieces))
        level = level * jnp.repeat(jnp.exp(draws), shape[dim] // shards_of).reshape((-1,) + (1,) * (len(shape) - 1 - dim))
    return level


def assign_block(key, own, number, rows, count, top, bound, slope):
    ranking = jax.random.permutation(key, count)
    crowded, usual = portions_of(count, rows * top, bound, slope, True), portions_of(count, rows * top, bound, slope, False)
    places = jnp.arange(count)

    def named(lengths, turn):
        used = int((lengths > 0).sum())
        fixed = max(1, used // 4)
        passed = fixed + (places - fixed + turn * (used - fixed)) % max(1, count - fixed)
        return jnp.zeros((count,), jnp.int32).at[ranking[jnp.where(places < fixed, places, passed)]].set(jnp.asarray(lengths, jnp.int32))

    lengths = jnp.where(number % 4 == 0, named(crowded, number // 4), named(usual, number - number // 4 - 1))
    mixed = jax.random.permutation(jax.random.fold_in(own, 3), count)
    donor, taker = mixed[0:count // 2 * 2:2], mixed[1:count // 2 * 2:2]
    room = jnp.minimum(lengths[donor] - 1, bound - lengths[taker]) // 2
    room = jnp.where((donor == ranking[0]) | (taker == ranking[0]) | (lengths[taker] == 0), 0, jnp.maximum(room, 0))
    passed = jax.random.randint(jax.random.fold_in(own, 4), (count // 2,), 0, 1 << 20) % (room + 1)
    lengths = lengths.at[donor].add(-passed).at[taker].add(passed)
    members = jnp.searchsorted(jnp.cumsum(lengths), jnp.arange(rows * top), side="right").astype(jnp.int32)
    listing = members.reshape(top, rows).T
    listing = listing[jax.random.permutation(jax.random.fold_in(own, 1), rows)]
    turn = jax.random.randint(jax.random.fold_in(own, 2), (rows, 1), 0, top)
    return jnp.take_along_axis(listing, (jnp.arange(top)[None, :] + turn) % top, axis=1)


def portions_of(number_of, total, limit, skew, full):
    weights = [(1 << 20) // math.isqrt(grade ** skew) + 1 for grade in range(1, number_of + 1)]
    largest = limit if full else min(limit, max(-(-total // number_of), total * weights[0] // sum(weights)))
    least = 1 if total - largest >= number_of - 1 else 0
    counts, surplus = [largest] + [least] * (number_of - 1), total - largest - least * (number_of - 1)
    while surplus > 0:
        candidates = [i for i in range(1, number_of) if counts[i] < largest] or [i for i in range(1, number_of) if counts[i] < limit]
        mass, budget = sum([weights[i] for i in candidates]), surplus
        for i in candidates:
            extra = min(limit - counts[i], max(1, budget * weights[i] // mass), surplus)
            counts[i] = counts[i] + extra
            surplus = surplus - extra
    return np.array(counts)


def gaussian(rng, dims, width, most, split=(), kind=jnp.bfloat16):
    level = shard_levels(rng, dims, split, -0.22, 0.18) if split else 1.0
    values = jax.random.normal(rng, dims, jnp.float32) * width * level
    return jnp.minimum(jnp.maximum(values, -most), most).astype(kind)


def setup_inputs(seed: int = 0) -> dict:
    seeds = jax.random.split(jax.random.key(seed), 16)
    mixer_in = gaussian(seeds[0], (TOKENS, D), 1.0, 6.0, ((0, 128),))
    expert_in = gaussian(seeds[1], (EXP_TOKENS, D), 1.0, 6.0, ((0, 128),))
    mixer_gain = jnp.clip(1.0 + 0.18 * jax.random.normal(seeds[2], (D,), jnp.float32), 0.1, 1.9)
    query_weight = gaussian(seeds[3], (D, QHEADS * HEAD), D ** -0.5, 0.125)
    key_weight = gaussian(seeds[4], (D, KVHEADS * HEAD), D ** -0.5, 0.125)
    value_weight = gaussian(seeds[5], (D, KVHEADS * HEAD), D ** -0.5, 0.125)
    query_gain = draw_query_gain(jax.random.fold_in(seeds[15], 71), 0)
    key_gain = draw_key_gain(jax.random.fold_in(seeds[15], 71), 0)
    output_weight = gaussian(seeds[8], (QHEADS * HEAD, D), (QHEADS * HEAD) ** -0.5, 0.1875)
    expert_gain = jnp.clip(1.0 + 0.18 * jax.random.normal(seeds[9], (D,), jnp.float32), 0.1, 1.9)
    routes_keys = jax.random.split(jax.random.fold_in(seeds[10], 1), EXP_TOKENS // EXP_TOK)
    routes_turns = jax.random.permutation(jax.random.fold_in(seeds[10], 3), EXP_TOKENS // EXP_TOK)
    routes = jax.vmap(lambda own, number: assign_block(jax.random.fold_in(seeds[10], 2), own, number, EXP_TOK, EXPERTS, TOPK, CAP, 2))(routes_keys, routes_turns).reshape((EXP_TOKENS, TOPK))
    route_weight = jnp.clip(0.2 + 1.3 * jax.random.uniform(seeds[11], (EXP_TOKENS, TOPK), jnp.float32) ** shard_levels(seeds[11], (EXP_TOKENS, TOPK), ((0, 128),), -0.2, 0.2), 0.2, 1.5)
    gate_weight = gaussian(seeds[12], (EXPERTS, D, FF), D ** -0.5, 0.125, ((0, 16),))
    up_weight = gaussian(seeds[13], (EXPERTS, D, FF), D ** -0.5, 0.125, ((0, 16),))
    down_weight = gaussian(seeds[14], (EXPERTS, FF, D), FF ** -0.5, 0.25, ((0, 16),))
    return {"mixer_in": mixer_in, "expert_in": expert_in, "mixer_gain": mixer_gain, "query_weight": query_weight, "key_weight": key_weight, "value_weight": value_weight, "query_gain": query_gain, "key_gain": key_gain, "output_weight": output_weight, "expert_gain": expert_gain, "routes": routes, "route_weight": route_weight, "gate_weight": gate_weight, "up_weight": up_weight, "down_weight": down_weight}


eps = 1e-06
theta = 10000.0

def row_norm(values, gain):
    values = values.astype(jnp.float32)
    scaled = values * lax.rsqrt(lax.optimization_barrier(jnp.mean(values * values, axis=-1, keepdims=True)) + eps)
    return scaled * gain.astype(jnp.float32)

def rotate(values, positions, grid):
    half = values.shape[-1] // 2
    freqs = half // 2
    inverse = theta ** (-(jnp.arange(freqs, dtype=jnp.float32) * 2.0) / half)
    grid_row = (positions // grid).astype(jnp.float32)
    grid_col = (positions % grid).astype(jnp.float32)
    angles = jnp.concatenate([grid_row[:, None] * inverse, grid_col[:, None] * inverse], axis=-1)
    cosine = jnp.cos(angles)[:, None, :]
    sine = jnp.sin(angles)[:, None, :]
    first = values[..., :half]
    second = values[..., half:]
    return jnp.concatenate([first * cosine - second * sine, second * cosine + first * sine], axis=-1)

def project(rows, positions, mixer_gain, query_weight, key_weight, value_weight, query_gain, key_gain):
    count = rows.shape[0]
    normed = row_norm(rows, mixer_gain).astype(jnp.bfloat16)
    queries = jnp.dot(normed, query_weight, preferred_element_type=jnp.float32).reshape(count, QHEADS, HEAD)
    keys = jnp.dot(normed, key_weight, preferred_element_type=jnp.float32).reshape(count, KVHEADS, HEAD)
    values = jnp.dot(normed, value_weight, preferred_element_type=jnp.float32).astype(jnp.bfloat16)
    queries = rotate(row_norm(queries, query_gain), positions, GRID).astype(jnp.bfloat16)
    keys = rotate(row_norm(keys, key_gain), positions, GRID).astype(jnp.bfloat16)
    return (queries, jnp.concatenate([keys.reshape(count, KVHEADS * HEAD), values], axis=1))

def reference(mixer_in, expert_in, mixer_gain, query_weight, key_weight, value_weight, query_gain, key_gain, output_weight, expert_gain, routes, route_weight, gate_weight, up_weight, down_weight):
    positions = jnp.arange(TOKENS, dtype=jnp.int32)
    queries, keyvals = project(mixer_in, positions, mixer_gain, query_weight, key_weight, value_weight, query_gain, key_gain)
    keys = keyvals[:, :KVHEADS * HEAD].reshape(TOKENS, KVHEADS, HEAD).astype(jnp.float32)
    values = keyvals[:, KVHEADS * HEAD:].reshape(TOKENS, KVHEADS, HEAD).astype(jnp.float32)
    groups = QHEADS // KVHEADS
    block = math.gcd(TOKENS, 256)
    qblocks = queries.reshape(TOKENS // block, block, KVHEADS, groups, HEAD)

    def attend(qblock):
        scores = jnp.einsum('rkgd,pkd->kgrp', qblock.astype(jnp.float32), keys) * HEAD ** (-0.5)
        peak = lax.optimization_barrier(jnp.max(scores, axis=-1, keepdims=True))
        expd = jnp.exp(scores - peak)
        total = lax.optimization_barrier(jnp.sum(expd, axis=-1))
        rounded = lax.optimization_barrier(expd.astype(jnp.bfloat16)).astype(jnp.float32)
        numer = jnp.einsum('kgrp,pkd->kgrd', rounded, values)
        out = numer / total[..., None]
        return jnp.transpose(out, (2, 0, 1, 3)).astype(jnp.bfloat16)
    attended = lax.map(attend, qblocks).reshape(TOKENS, QHEADS * HEAD)
    mixer_out = jnp.dot(attended, output_weight, preferred_element_type=jnp.float32).astype(jnp.bfloat16)
    normed = row_norm(expert_in, expert_gain).astype(jnp.bfloat16)
    holders = N_EP * N_TP
    entries = EXP_TOKENS * TOPK
    flat = routes.reshape(-1).astype(jnp.int32)
    hot = (flat[:, None] == jnp.arange(EXPERTS, dtype=jnp.int32)[None, :]).astype(jnp.int32)
    blocks = hot.reshape(holders, EXP_TOK * TOPK, EXPERTS)
    before = (jnp.cumsum(blocks, axis=1) - blocks).reshape(entries, EXPERTS)
    rank = lax.optimization_barrier(jnp.sum(before * hot, axis=-1)).astype(jnp.int32)
    holder_of = (jnp.arange(entries, dtype=jnp.int32) // (EXP_TOK * TOPK)).astype(jnp.int32)
    slot = (flat * (holders * CAP) + holder_of * CAP + rank).astype(jnp.int32)
    source = (jnp.arange(entries, dtype=jnp.int32) // TOPK).astype(jnp.int32)
    table = jnp.full((EXPERTS * holders * CAP,), EXP_TOKENS, jnp.int32).at[slot].set(source)
    padded = jnp.concatenate([normed, jnp.zeros((1, D), jnp.bfloat16)], axis=0)

    def expert(index):
        chosen = padded[lax.dynamic_slice_in_dim(table, index * (holders * CAP), holders * CAP)]
        gate = jnp.dot(chosen, gate_weight[index], preferred_element_type=jnp.float32)
        upper = jnp.dot(chosen, up_weight[index], preferred_element_type=jnp.float32)
        hidden = (jax.nn.silu(gate) * upper).astype(jnp.bfloat16)
        return jnp.dot(hidden, down_weight[index], preferred_element_type=jnp.float32).astype(jnp.bfloat16)
    results = lax.map(expert, jnp.arange(EXPERTS, dtype=jnp.int32))
    picked = results.reshape(EXPERTS * holders * CAP, D)[slot].reshape(EXP_TOKENS, TOPK, D)
    expert_out = lax.optimization_barrier(jnp.sum(picked.astype(jnp.float32) * route_weight.astype(jnp.float32)[..., None], axis=1)).astype(jnp.bfloat16)
    return (mixer_out, expert_out)
```

```python
import functools

import jax
import jax.numpy as jnp
from jax import lax
from jax.experimental import pallas as pl
from jax.experimental.pallas import tpu as pltpu
from jax.sharding import PartitionSpec as P


D = 2048
HEAD = 64
QHEADS = 16
KVHEADS = 2
GRID = 64
FF = 512
EXP_DEV = 2
CAP = 64
LANES = 128
KEY_BLOCK = 2048
ROW_TILE = 256
VMEM = 56 * 1024 * 1024

eps = 1e-06
theta = 10000.0

f32 = jnp.float32
bf16 = jnp.bfloat16


def params(*semantics):
    return pltpu.CompilerParams(
        dimension_semantics=semantics or None, vmem_limit_bytes=VMEM
    )


def cost(flops, moved):
    return pl.CostEstimate(flops=int(flops), transcendentals=0, bytes_accessed=int(moved))


def normed_rows(values, gain):
    values = values.astype(f32)
    scaled = values * lax.rsqrt(jnp.mean(values * values, axis=-1, keepdims=True) + eps)
    return (scaled * gain).astype(bf16)


def head_pair(u, gain, cosine, sine):
    lane = lax.broadcasted_iota(jnp.int32, u.shape, 1)
    left = lane < HEAD
    square = u * u
    first = jnp.sum(jnp.where(left, square, 0.0), axis=-1, keepdims=True)
    second = jnp.sum(jnp.where(left, 0.0, square), axis=-1, keepdims=True)
    mean = jnp.where(left, first, second) * (1.0 / HEAD)
    u = u * lax.rsqrt(mean + eps) * gain
    half = HEAD // 2
    swapped = jnp.where(
        lane % HEAD < half, pltpu.roll(u, LANES - half, 1), pltpu.roll(u, half, 1)
    )
    return u * cosine + swapped * sine


def keyval_body(x_ref, gain_ref, kw_ref, vw_ref, kgain_ref, cos_ref, sin_ref, out_ref):
    normed = normed_rows(x_ref[...], gain_ref[...])
    keys = jnp.dot(normed, kw_ref[...], preferred_element_type=f32)
    values = jnp.dot(normed, vw_ref[...], preferred_element_type=f32)
    out_ref[:, :LANES] = head_pair(keys, kgain_ref[...], cos_ref[...], sin_ref[...]).astype(bf16)
    out_ref[:, LANES:] = values.astype(bf16)


def query_body(x_ref, gain_ref, qw_ref, qgain_ref, cos_ref, sin_ref, out_ref):
    normed = normed_rows(x_ref[...], gain_ref[...])
    rows = x_ref.shape[0]
    left = lax.broadcasted_iota(jnp.int32, (rows, LANES), 1) < HEAD
    scale = HEAD ** (-0.5)
    for pair in range(QHEADS // 2):
        u = jnp.dot(
            normed, qw_ref[:, pair * LANES : (pair + 1) * LANES], preferred_element_type=f32
        )
        u = head_pair(u, qgain_ref[...], cos_ref[...], sin_ref[...])
        u = u.astype(bf16).astype(f32) * scale
        moved = pltpu.roll(u, HEAD, 1)
        for odd in range(2):
            head = 2 * pair + odd
            group = head // (QHEADS // KVHEADS)
            source = u if odd == group else moved
            keep = left if group == 0 else jnp.logical_not(left)
            out_ref[head * rows : (head + 1) * rows, :] = jnp.where(keep, source, 0.0).astype(bf16)


def attend_body(q_ref, kv_ref, out_ref, peak_ref, acc_ref, *, own, group):
    step = pl.program_id(0)

    @pl.when(step == 0)
    def _():
        peak_ref[...] = jnp.full(peak_ref.shape, -jnp.inf, f32)
        acc_ref[...] = jnp.zeros(acc_ref.shape, f32)

    keys = kv_ref[:, :LANES]
    values = jnp.concatenate(
        [kv_ref[:, LANES:], jnp.ones((kv_ref.shape[0], LANES), bf16)], axis=1
    )

    def tile(start):
        rows = pl.ds(start, ROW_TILE)
        scores = lax.dot_general(
            q_ref[rows, :], keys, (((1,), (1,)), ((), ())), preferred_element_type=f32
        )
        before = peak_ref[rows, :1]
        fresh = jnp.maximum(before, jnp.max(scores, axis=-1, keepdims=True))
        factor = jnp.exp(before - fresh)
        weights = jnp.exp(scores - fresh).astype(bf16)
        peak_ref[rows, :] = jnp.broadcast_to(fresh, (ROW_TILE, LANES))
        acc_ref[rows, :] = acc_ref[rows, :] * factor + jnp.dot(
            weights, values, preferred_element_type=f32
        )

    def pair(index, carry):
        start = pl.multiple_of(index * (2 * ROW_TILE), 2 * ROW_TILE)
        tile(start)
        tile(start + ROW_TILE)
        return carry

    lax.fori_loop(0, q_ref.shape[0] // (2 * ROW_TILE), pair, 0)

    @pl.when(step == pl.num_programs(0) - 1)
    def _():
        left = lax.broadcasted_iota(jnp.int32, (own, LANES), 1) < HEAD
        for two in range(q_ref.shape[0] // (2 * own)):
            done = []
            for head in (2 * two, 2 * two + 1):
                block = acc_ref[head * own : (head + 1) * own, :]
                done.append(block[:, :LANES] / block[:, LANES:])
            if group == 0:
                both = jnp.where(left, done[0], pltpu.roll(done[1], HEAD, 1))
            else:
                both = jnp.where(left, pltpu.roll(done[0], HEAD, 1), done[1])
            out_ref[:, two * LANES : (two + 1) * LANES] = both.astype(bf16)


def attend(queries, keyvals, own, group):
    rows, keys = queries.shape[0] // KVHEADS, keyvals.shape[0]
    width = rows // own * HEAD
    return pl.pallas_call(
        functools.partial(attend_body, own=own, group=group),
        grid=(keys // KEY_BLOCK,),
        in_specs=[
            pl.BlockSpec((rows, LANES), lambda i: (group, 0)),
            pl.BlockSpec((KEY_BLOCK, 2 * LANES), lambda i: (i, 0)),
        ],
        out_specs=pl.BlockSpec((own, width), lambda i: (0, 0)),
        out_shape=jax.ShapeDtypeStruct((own, width), bf16),
        scratch_shapes=[
            pltpu.VMEM((rows, LANES), f32),
            pltpu.VMEM((rows, 2 * LANES), f32),
        ],
        compiler_params=params("arbitrary"),
        cost_estimate=cost(rows * keys * 1024, keys * 512),
        name="attend",
    )(queries, keyvals)


def route_body(x_ref, gain_ref, routes_ref, weights_ref, normed_ref, place_ref, spot_ref, share_ref):
    normed_ref[...] = normed_rows(x_ref[...], gain_ref[...])
    tokens, experts = spot_ref.shape
    expert = lax.broadcasted_iota(jnp.int32, (tokens, experts), 1)
    one = routes_ref[:, 0:1] == expert
    two = routes_ref[:, 1:2] == expert
    share_ref[...] = jnp.where(one, weights_ref[:, 0:1], 0.0) + jnp.where(
        two, weights_ref[:, 1:2], 0.0
    )
    named = jnp.where(jnp.logical_or(one, two), 1.0, 0.0)
    count = named.astype(bf16)
    row = lax.broadcasted_iota(jnp.int32, (tokens, tokens), 0)
    col = lax.broadcasted_iota(jnp.int32, (tokens, tokens), 1)
    earlier = jnp.where(col < row, 1.0, 0.0).astype(bf16)
    before = jnp.dot(earlier, count, preferred_element_type=f32)
    spot = jnp.where(named > 0.0, before, -1.0)
    spot_ref[...] = spot
    place_ref[...] = spot.T


def route(rows, gain, routes, weights, experts):
    tokens = rows.shape[0]
    return pl.pallas_call(
        route_body,
        out_shape=(
            jax.ShapeDtypeStruct((tokens, D), bf16),
            jax.ShapeDtypeStruct((experts, tokens), f32),
            jax.ShapeDtypeStruct((tokens, experts), f32),
            jax.ShapeDtypeStruct((tokens, experts), f32),
        ),
        compiler_params=params(),
        cost_estimate=cost(tokens * D * 100, tokens * D * 4),
        name="route",
    )(rows, gain, routes, weights)


def dispatch_body(place_ref, normed_ref, out_ref, pick_ref, *, which):
    experts, tokens = place_ref.shape
    owners = experts // EXP_DEV

    @pl.when(pl.program_id(0) == 0)
    def _():
        slot = lax.broadcasted_iota(jnp.int32, (CAP, tokens), 0).astype(f32)
        for owner in range(owners):
            expert = owner * EXP_DEV + which
            pick_ref[owner * CAP : (owner + 1) * CAP, :] = jnp.where(
                place_ref[expert : expert + 1, :] == slot, 1.0, 0.0
            ).astype(bf16)

    rows = jnp.dot(pick_ref[...], normed_ref[...], preferred_element_type=f32).astype(bf16)
    out_ref[...] = rows.reshape(out_ref.shape)


def dispatch(place, normed, which):
    experts, tokens = place.shape
    owners = experts // EXP_DEV
    block = 512
    return pl.pallas_call(
        functools.partial(dispatch_body, which=which),
        grid=(D // block,),
        in_specs=[
            pl.BlockSpec((experts, tokens), lambda i: (0, 0)),
            pl.BlockSpec((tokens, block), lambda i: (0, i)),
        ],
        out_specs=pl.BlockSpec((owners, CAP, block), lambda i: (0, 0, i)),
        out_shape=jax.ShapeDtypeStruct((owners, CAP, D), bf16),
        scratch_shapes=[pltpu.VMEM((owners * CAP, tokens), bf16)],
        compiler_params=params("arbitrary"),
        cost_estimate=cost(2 * owners * CAP * tokens * D, 6 * 2**20),
        name="dispatch",
    )(place, normed)


def expert_body(x_ref, gate_ref, up_ref, down_ref, out_ref):
    rows = x_ref[...].reshape(-1, D)
    gate = jnp.dot(rows, gate_ref[0], preferred_element_type=f32)
    upper = jnp.dot(rows, up_ref[0], preferred_element_type=f32)
    hidden = (gate * (1.0 / (1.0 + jnp.exp(-gate))) * upper).astype(bf16)
    out_ref[...] = (
        jnp.dot(hidden, down_ref[0], preferred_element_type=f32).astype(bf16).reshape(out_ref.shape)
    )


def expert(rows, gate, up, down, which):
    sources = rows.shape[0]
    tile = 4
    return pl.pallas_call(
        expert_body,
        grid=(sources // tile,),
        in_specs=[
            pl.BlockSpec((tile, CAP, D), lambda i: (i, 0, 0)),
            pl.BlockSpec((1, D, FF), lambda i: (which, 0, 0)),
            pl.BlockSpec((1, D, FF), lambda i: (which, 0, 0)),
            pl.BlockSpec((1, FF, D), lambda i: (which, 0, 0)),
        ],
        out_specs=pl.BlockSpec((tile, CAP, D), lambda i: (i, 0, 0)),
        out_shape=jax.ShapeDtypeStruct(rows.shape, bf16),
        compiler_params=params("arbitrary"),
        cost_estimate=cost(6 * sources * CAP * D * FF, 14 * 2**20),
        name="expert",
    )(rows, gate, up, down)


def combine_body(*refs, which, last):
    if last:
        spot_ref, share_ref, back_ref, part_ref, out_ref, high_ref, low_ref = refs
    else:
        spot_ref, share_ref, back_ref, out_ref, high_ref, low_ref = refs
    tokens, experts = spot_ref.shape

    @pl.when(pl.program_id(0) == 0)
    def _():
        lane = lax.broadcasted_iota(jnp.int32, (tokens, LANES), 1)
        left = lane < CAP
        slot = (lane % CAP).astype(f32)
        for two in range(experts // (2 * EXP_DEV)):
            near = 2 * two * EXP_DEV + which
            far = near + EXP_DEV
            spot = jnp.where(left, spot_ref[:, near : near + 1], spot_ref[:, far : far + 1])
            share = jnp.where(left, share_ref[:, near : near + 1], share_ref[:, far : far + 1])
            weight = jnp.where(spot == slot, share, 0.0)
            high = weight.astype(bf16)
            high_ref[:, two * LANES : (two + 1) * LANES] = high
            low_ref[:, two * LANES : (two + 1) * LANES] = (weight - high.astype(f32)).astype(bf16)

    back = back_ref[...].reshape(-1, back_ref.shape[-1])
    total = jnp.dot(high_ref[...], back, preferred_element_type=f32)
    total = total + jnp.dot(low_ref[...], back, preferred_element_type=f32)
    if last:
        total = total + part_ref[...]
    out_ref[...] = total.astype(out_ref.dtype)


def combine(spot, share, back, part, which):
    tokens, experts = spot.shape
    owners = experts // EXP_DEV
    last = part is not None
    block = 512
    small = pl.BlockSpec((tokens, experts), lambda i: (0, 0))
    column = pl.BlockSpec((tokens, block), lambda i: (0, i))
    specs = [small, small, pl.BlockSpec((owners, CAP, block), lambda i: (0, 0, i))]
    operands = [spot, share, back]
    if last:
        specs.append(column)
        operands.append(part)
    return pl.pallas_call(
        functools.partial(combine_body, which=which, last=last),
        grid=(D // block,),
        in_specs=specs,
        out_specs=column,
        out_shape=jax.ShapeDtypeStruct((tokens, D), bf16 if last else f32),
        scratch_shapes=[pltpu.VMEM((tokens, owners * CAP), bf16)] * 2,
        compiler_params=params("arbitrary"),
        cost_estimate=cost(4 * owners * CAP * tokens * D, 8 * 2**20),
        name="combine",
    )(*operands)


def tables(offset, count):
    lane = jnp.arange(LANES, dtype=jnp.int32)[None, :] + jnp.zeros((count, 1), jnp.int32)
    position = offset + jnp.arange(count, dtype=jnp.int32)[:, None] + jnp.zeros_like(lane)
    half = HEAD // 2
    freqs = half // 2
    inverse = theta ** (-((lane % freqs).astype(f32) * 2.0) / half)
    place = jnp.where(lane % half < freqs, position // GRID, position % GRID).astype(f32)
    angles = place * inverse
    sine = jnp.sin(angles)
    return jnp.cos(angles), jnp.where(lane % HEAD < half, -sine, sine)


def per_device(
    mixer_in,
    expert_in,
    mixer_gain,
    query_weight,
    key_weight,
    value_weight,
    query_gain,
    key_gain,
    output_weight,
    expert_gain,
    routes,
    route_weight,
    gate_weight,
    up_weight,
    down_weight,
):
    own = mixer_in.shape[0]
    offset = (lax.axis_index("ep") * lax.axis_size("tp") + lax.axis_index("tp")) * own
    cosine, sine = tables(offset, own)
    gain = mixer_gain.reshape(1, D)
    kgain = jnp.tile(key_gain, 2).reshape(1, LANES)
    qgain = jnp.tile(query_gain, 2).reshape(1, LANES)
    keyvals = pl.pallas_call(
        keyval_body,
        out_shape=jax.ShapeDtypeStruct((own, 2 * LANES), bf16),
        compiler_params=params(),
        cost_estimate=cost(own * D * 512, 2 * 2**20),
        name="keyval",
    )(mixer_in, gain, key_weight, value_weight, kgain, cosine, sine)
    everyone = lax.all_gather(keyvals, ("ep", "tp"), axis=0, tiled=True)

    experts = EXP_DEV * lax.axis_size("ep")
    normed, place, spot, share = route(
        expert_in, expert_gain.reshape(1, D), routes, route_weight, experts
    )

    def exchange(rows):
        return lax.all_to_all(rows, "ep", split_axis=0, concat_axis=0, tiled=True)

    arrived = [exchange(dispatch(place, normed, which)) for which in range(EXP_DEV)]
    queries = pl.pallas_call(
        query_body,
        out_shape=jax.ShapeDtypeStruct((QHEADS * own, LANES), bf16),
        compiler_params=params(),
        cost_estimate=cost(own * D * 2048, 5 * 2**20),
        name="query",
    )(mixer_in, gain, query_weight, qgain, cosine, sine)
    returned = []
    for which in range(EXP_DEV):
        result = expert(arrived[which], gate_weight, up_weight, down_weight, which)
        returned.append(exchange(result))
    pieces = []
    for group in range(KVHEADS):
        pieces.append(attend(queries, everyone, own, group))
    part = combine(spot, share, returned[0], None, 0)
    attended = jnp.concatenate(pieces, axis=1)
    mixer_out = jnp.dot(attended, output_weight, preferred_element_type=f32).astype(bf16)
    expert_out = combine(spot, share, returned[1], part, 1)
    return (mixer_out, expert_out)


def solution(mesh):
    placed = (
        P(("ep", "tp"), None),
        P(("ep", "tp"), None),
        P(),
        P(),
        P(),
        P(),
        P(),
        P(),
        P(),
        P(),
        P(("ep", "tp"), None),
        P(("ep", "tp"), None),
        P("ep", None, None),
        P("ep", None, None),
        P("ep", None, None),
    )

    return jax.shard_map(
        per_device,
        mesh=mesh,
        in_specs=placed,
        out_specs=(P(("ep", "tp"), None), P(("ep", "tp"), None)),
        check_vma=False,
    )
```

```python
import functools

import jax
import jax.numpy as jnp
from jax import lax
from jax.experimental import pallas as pl
from jax.experimental.pallas import tpu as pltpu
from jax.sharding import PartitionSpec as P


D = 2048
HEAD = 64
QHEADS = 16
KVHEADS = 2
GRID = 64
FF = 512
TOPK = 2
EXP_DEV = 2
CAP = 64
LANES = 128
KEY_BLOCK = 2048
ROW_TILE = 512
SIDE = 4
GROUPS = ((0, 10, 6, 14, 9, 11), (5, 15, 7, 13, 2, 8), (1, 3, 4, 12))
SAFE_LIMIT = 60.0
VMEM = 56 * 1024 * 1024

eps = 1e-06
theta = 10000.0
LOG2_E = 1.4426950408889634

f32 = jnp.float32
bf16 = jnp.bfloat16


def params(*semantics):
    return pltpu.CompilerParams(
        dimension_semantics=semantics or None, vmem_limit_bytes=VMEM
    )


def cost(flops, moved):
    return pl.CostEstimate(flops=int(flops), transcendentals=0, bytes_accessed=int(moved))


def normed_rows(values, gain):
    values = values.astype(f32)
    scaled = values * lax.rsqrt(jnp.mean(values * values, axis=-1, keepdims=True) + eps)
    return (scaled * gain).astype(bf16)


def head_pair(u, gain, cosine, sine):
    lane = lax.broadcasted_iota(jnp.int32, u.shape, 1)
    left = lane < HEAD
    square = u * u
    first = jnp.sum(jnp.where(left, square, 0.0), axis=-1, keepdims=True)
    second = jnp.sum(jnp.where(left, 0.0, square), axis=-1, keepdims=True)
    mean = jnp.where(left, first, second) * (1.0 / HEAD)
    u = u * lax.rsqrt(mean + eps) * gain
    half = HEAD // 2
    swapped = jnp.where(
        lane % HEAD < half, pltpu.roll(u, LANES - half, 1), pltpu.roll(u, half, 1)
    )
    return u * cosine + swapped * sine


def twice(gain):
    return jnp.concatenate([gain, gain], axis=1)


def keyval_body(x_ref, gain_ref, kw_ref, vw_ref, kgain_ref, cos_ref, sin_ref, out_ref):
    normed = normed_rows(x_ref[...], gain_ref[...])
    keys = jnp.dot(normed, kw_ref[...], preferred_element_type=f32)
    values = jnp.dot(normed, vw_ref[...], preferred_element_type=f32)
    out_ref[:, :LANES] = head_pair(keys, twice(kgain_ref[...]), cos_ref[...], sin_ref[...]).astype(bf16)
    out_ref[:, LANES:] = values.astype(bf16)


def query_body(x_ref, gain_ref, qw_ref, qgain_ref, cos_ref, sin_ref, out_ref):
    normed = normed_rows(x_ref[...], gain_ref[...])
    rows = x_ref.shape[0]
    left = lax.broadcasted_iota(jnp.int32, (rows, LANES), 1) < HEAD
    qgain = twice(qgain_ref[...])
    scale = HEAD ** (-0.5) * LOG2_E
    for pair in range(QHEADS // 2):
        u = jnp.dot(
            normed, qw_ref[:, pair * LANES : (pair + 1) * LANES], preferred_element_type=f32
        )
        u = head_pair(u, qgain, cos_ref[...], sin_ref[...])
        u = u.astype(bf16).astype(f32) * scale
        moved = pltpu.roll(u, HEAD, 1)
        for odd in range(2):
            head = 2 * pair + odd
            group = head // (QHEADS // KVHEADS)
            source = u if odd == group else moved
            keep = left if group == 0 else jnp.logical_not(left)
            source = jnp.where(keep, source, 0.0)
            high = source.astype(bf16)
            place = slice(head * rows, (head + 1) * rows)
            out_ref[place, :LANES] = high
            out_ref[place, LANES:] = (source - high.astype(f32)).astype(bf16)


def attend_body(safe_ref, q_ref, kv_ref, *refs, own, first, last):
    step = pl.program_id(0)
    if last:
        out_ref, peak_ref, acc_ref = refs[-3:]
    else:
        peak_ref, acc_ref = refs[-2:]

    @pl.when(step == 0)
    def _():
        if first:
            peak_ref[...] = jnp.full(peak_ref.shape, -jnp.inf, f32)
            acc_ref[...] = jnp.zeros(acc_ref.shape, f32)
        else:
            peak_ref[...] = refs[0][...]
            acc_ref[...] = refs[1][...]

    keys = kv_ref[:, :LANES]
    keys = jnp.concatenate([keys, keys], axis=1)
    values = kv_ref[:, LANES:]
    values = jnp.concatenate([values, jnp.ones(values.shape, bf16)], axis=1)

    def score(rows):
        return lax.dot_general(
            q_ref[rows, :], keys, (((1,), (1,)), ((), ())), preferred_element_type=f32
        )

    def gather(weights):
        return jnp.dot(weights.astype(bf16), values, preferred_element_type=f32)

    def plain(rows):
        acc_ref[rows, :] += gather(jnp.exp2(score(rows)))

    def careful(rows):
        scores = score(rows)
        before = peak_ref[rows, :1]
        fresh = jnp.maximum(before, jnp.max(scores, axis=-1, keepdims=True))
        peak_ref[rows, :] = jnp.broadcast_to(fresh, (fresh.shape[0], LANES))
        acc_ref[rows, :] = acc_ref[rows, :] * jnp.exp2(before - fresh) + gather(
            jnp.exp2(scores - fresh)
        )

    def sweep(work, tile, times):
        def some(index, carry):
            for time in range(times):
                start = pl.multiple_of((index * times + time) * tile, tile)
                work(pl.ds(start, tile))
            return carry

        lax.fori_loop(0, q_ref.shape[0] // (tile * times), some, 0)

    safe = safe_ref[0] <= SAFE_LIMIT

    @pl.when(safe)
    def _():
        sweep(plain, ROW_TILE, 2)

    @pl.when(jnp.logical_not(safe))
    def _():
        sweep(careful, ROW_TILE // 8, 1)

    if not last:
        return

    @pl.when(step == pl.num_programs(0) - 1)
    def _():
        left = lax.broadcasted_iota(jnp.int32, (own, LANES), 1) < HEAD
        for two in range(QHEADS // 2):
            done = []
            for head in (2 * two, 2 * two + 1):
                block = acc_ref[head * own : (head + 1) * own, :]
                done.append(block[:, :LANES] / block[:, LANES:])
            if 2 * two < QHEADS // KVHEADS:
                both = jnp.where(left, done[0], pltpu.roll(done[1], HEAD, 1))
            else:
                both = jnp.where(left, pltpu.roll(done[0], HEAD, 1), done[1])
            out_ref[:, two * LANES : (two + 1) * LANES] = both.astype(bf16)


def attend(safe, queries, keyvals, state, own, last):
    rows, keys = queries.shape[0], keyvals.shape[0]
    whole = lambda i: (0, 0)
    carried = [pl.BlockSpec((rows, LANES), whole), pl.BlockSpec((rows, 2 * LANES), whole)]
    shapes = [
        jax.ShapeDtypeStruct((rows, LANES), f32),
        jax.ShapeDtypeStruct((rows, 2 * LANES), f32),
    ]
    first = state is None
    return pl.pallas_call(
        functools.partial(attend_body, own=own, first=first, last=last),
        grid=(keys // KEY_BLOCK,),
        in_specs=[
            pl.BlockSpec(memory_space=pltpu.SMEM),
            pl.BlockSpec((rows, 2 * LANES), whole),
            pl.BlockSpec((KEY_BLOCK, 2 * LANES), lambda i: (i, 0)),
        ]
        + ([] if first else carried),
        out_specs=pl.BlockSpec((own, QHEADS * HEAD), whole) if last else carried,
        out_shape=jax.ShapeDtypeStruct((own, QHEADS * HEAD), bf16) if last else shapes,
        scratch_shapes=[pltpu.VMEM(shape.shape, f32) for shape in shapes] if last else [],
        compiler_params=params("arbitrary"),
        cost_estimate=cost(rows * keys * 1024, keys * 512),
        name="attend",
    )(safe, queries, keyvals, *([] if first else state))


def fill_pick(place_ref, pick_ref, group):
    slot = lax.broadcasted_iota(jnp.int32, (CAP, place_ref.shape[1]), 0).astype(f32)
    for index, shift in enumerate(group):
        for which in range(EXP_DEV):
            row = shift * EXP_DEV + which
            start = (index * EXP_DEV + which) * CAP
            pick_ref[start : start + CAP, :] = jnp.where(
                place_ref[row : row + 1, :] == slot, 1.0, 0.0
            ).astype(bf16)


def pick_rows(pick_ref, normed, out_refs):
    rows = jnp.dot(pick_ref[...], normed, preferred_element_type=f32).astype(bf16)
    span = EXP_DEV * CAP
    for index, out_ref in enumerate(out_refs):
        out_ref[...] = rows[index * span : (index + 1) * span].reshape(out_ref.shape)


def relative(routes, here_ref):
    holder = routes // EXP_DEV
    down = (holder // SIDE - here_ref[0] + SIDE) % SIDE
    across = (holder % SIDE - here_ref[1] + SIDE) % SIDE
    return (down * SIDE + across) * EXP_DEV + routes % EXP_DEV


def route_body(here_ref, x_ref, gain_ref, routes_ref, *refs, group):
    out_refs, (normed_ref, place_ref, named_ref, pick_ref) = refs[:-4], refs[-4:]
    step = pl.program_id(0)
    experts, tokens = place_ref.shape
    block = out_refs[0].shape[-1]

    @pl.when(step == 0)
    def _():
        named_ref[...] = relative(routes_ref[...], here_ref)
        expert = lax.broadcasted_iota(jnp.int32, (experts, tokens), 0)
        one = named_ref[0:1, :] == expert
        two = named_ref[1:2, :] == expert
        named = jnp.where(jnp.logical_or(one, two), 1.0, 0.0)
        row = lax.broadcasted_iota(jnp.int32, (tokens, tokens), 0)
        col = lax.broadcasted_iota(jnp.int32, (tokens, tokens), 1)
        earlier = jnp.where(row < col, 1.0, 0.0).astype(bf16)
        before = jnp.dot(named.astype(bf16), earlier, preferred_element_type=f32)
        place_ref[...] = jnp.where(named > 0.0, before, -1.0)
        fill_pick(place_ref, pick_ref, group)
        normed_ref[...] = normed_rows(x_ref[...], gain_ref[...])

    start = pl.multiple_of(step * block, block)
    pick_rows(pick_ref, normed_ref[:, pl.ds(start, block)], out_refs)


def bundles(count, block):
    return (
        [pl.BlockSpec((EXP_DEV, CAP, block), lambda i: (0, 0, i))] * count,
        [jax.ShapeDtypeStruct((EXP_DEV, CAP, D), bf16)] * count,
    )


def route(here, rows, gain, routes, experts, group):
    tokens = rows.shape[0]
    block = 512
    specs, shapes = bundles(len(group), block)
    whole = lambda i: (0, 0)
    return pl.pallas_call(
        functools.partial(route_body, group=group),
        grid=(D // block,),
        in_specs=[
            pl.BlockSpec(memory_space=pltpu.SMEM),
            pl.BlockSpec((tokens, D), whole),
            pl.BlockSpec((1, D), whole),
            pl.BlockSpec((TOPK, tokens), whole),
        ],
        out_specs=specs
        + [
            pl.BlockSpec((tokens, D), whole),
            pl.BlockSpec((experts, tokens), whole),
            pl.BlockSpec((TOPK, tokens), whole),
        ],
        out_shape=shapes
        + [
            jax.ShapeDtypeStruct((tokens, D), bf16),
            jax.ShapeDtypeStruct((experts, tokens), f32),
            jax.ShapeDtypeStruct((TOPK, tokens), jnp.int32),
        ],
        scratch_shapes=[pltpu.VMEM((len(group) * EXP_DEV * CAP, tokens), bf16)],
        compiler_params=params("arbitrary"),
        cost_estimate=cost(8e9, 8 * 2**20),
        name="route",
    )(here, rows, gain, routes)


def dispatch_body(place_ref, normed_ref, *refs, group):
    out_refs, pick_ref = refs[:-1], refs[-1]

    @pl.when(pl.program_id(0) == 0)
    def _():
        fill_pick(place_ref, pick_ref, group)

    pick_rows(pick_ref, normed_ref[...], out_refs)


def dispatch(place, normed, group):
    experts, tokens = place.shape
    block = 512
    specs, shapes = bundles(len(group), block)
    return pl.pallas_call(
        functools.partial(dispatch_body, group=group),
        grid=(D // block,),
        in_specs=[
            pl.BlockSpec((experts, tokens), lambda i: (0, 0)),
            pl.BlockSpec((tokens, block), lambda i: (0, i)),
        ],
        out_specs=specs,
        out_shape=shapes,
        scratch_shapes=[pltpu.VMEM((len(group) * EXP_DEV * CAP, tokens), bf16)],
        compiler_params=params("arbitrary"),
        cost_estimate=cost(5e9, 6 * 2**20),
        name="dispatch",
    )(place, normed)


def shares_body(place_ref, named_ref, weights_ref, *out_refs):
    experts, tokens = place_ref.shape
    expert = lax.broadcasted_iota(jnp.int32, (experts, tokens), 0)
    share = jnp.where(named_ref[0:1, :] == expert, weights_ref[0:1, :], 0.0) + jnp.where(
        named_ref[1:2, :] == expert, weights_ref[1:2, :], 0.0
    )
    slot = lax.broadcasted_iota(jnp.int32, (CAP, tokens), 0).astype(f32)
    for group, out_ref in zip(GROUPS, out_refs):
        for index, shift in enumerate(group):
            tiles = []
            for which in range(EXP_DEV):
                row = slice(shift * EXP_DEV + which, shift * EXP_DEV + which + 1)
                tiles.append(jnp.where(place_ref[row, :] == slot, share[row, :], 0.0))
            value = jnp.concatenate(tiles, axis=0).T
            high = value.astype(bf16)
            low = (value - high.astype(f32)).astype(bf16)
            columns = slice(index * LANES, (index + 1) * LANES)
            out_ref[:tokens, columns] = high
            out_ref[tokens:, columns] = low


def shares(place, named, weights):
    tokens = place.shape[1]
    return pl.pallas_call(
        shares_body,
        out_shape=[
            jax.ShapeDtypeStruct((2 * tokens, len(group) * LANES), bf16) for group in GROUPS
        ],
        compiler_params=params(),
        cost_estimate=cost(4e9, 4 * 2**20),
        name="shares",
    )(place, named, weights)


def expert_body(gate_ref, up_ref, down_ref, *refs):
    count = len(refs) // 2
    rows = jnp.concatenate([ref[0] for ref in refs[:count]], axis=0)
    gate = jnp.dot(rows, gate_ref[0], preferred_element_type=f32)
    upper = jnp.dot(rows, up_ref[0], preferred_element_type=f32)
    hidden = (gate * (1.0 / (1.0 + jnp.exp(-gate))) * upper).astype(bf16)
    result = jnp.dot(hidden, down_ref[0], preferred_element_type=f32).astype(bf16)
    for index, out_ref in enumerate(refs[count:]):
        out_ref[0] = result[index * CAP : (index + 1) * CAP]


def expert(arrays, gate, up, down):
    each = lambda i: (i, 0, 0)
    count = len(arrays)
    rows = [pl.BlockSpec((1, CAP, D), each)] * count
    return pl.pallas_call(
        expert_body,
        grid=(EXP_DEV,),
        in_specs=[
            pl.BlockSpec((1, D, FF), each),
            pl.BlockSpec((1, D, FF), each),
            pl.BlockSpec((1, FF, D), each),
        ]
        + rows,
        out_specs=rows,
        out_shape=[jax.ShapeDtypeStruct((EXP_DEV, CAP, D), bf16)] * count,
        compiler_params=params("arbitrary"),
        cost_estimate=cost(6 * count * EXP_DEV * CAP * D * FF, 14 * 2**20),
        name="expert",
    )(gate, up, down, *arrays)


def combine_body(share_ref, *refs, first):
    out_ref = refs[-1]
    back_refs = refs[:-1] if first else refs[:-2]
    tokens = out_ref.shape[0]
    back = jnp.concatenate([ref[...].reshape(-1, ref.shape[-1]) for ref in back_refs], axis=0)
    both = jnp.dot(share_ref[...], back, preferred_element_type=f32)
    total = both[:tokens] + both[tokens:]
    if not first:
        total = total + refs[-2][...]
    out_ref[...] = total.astype(out_ref.dtype)


def combine(share, arrays, part, last):
    tokens = share.shape[0] // 2
    block = 512
    column = pl.BlockSpec((tokens, block), lambda i: (0, i))
    specs = [pl.BlockSpec(share.shape, lambda i: (0, 0))] + bundles(len(arrays), block)[0]
    operands = [share, *arrays]
    if part is not None:
        specs.append(column)
        operands.append(part)
    return pl.pallas_call(
        functools.partial(combine_body, first=part is None),
        grid=(D // block,),
        in_specs=specs,
        out_specs=column,
        out_shape=jax.ShapeDtypeStruct((tokens, D), bf16 if last else f32),
        compiler_params=params("arbitrary"),
        cost_estimate=cost(4 * share.shape[1] * tokens * D, 8 * 2**20),
        name="combine",
    )(*operands)


def tables(offset, count):
    lane = jnp.arange(LANES, dtype=jnp.int32)[None, :] + jnp.zeros((count, 1), jnp.int32)
    position = offset + jnp.arange(count, dtype=jnp.int32)[:, None] + jnp.zeros_like(lane)
    half = HEAD // 2
    freqs = half // 2
    inverse = theta ** (-((lane % freqs).astype(f32) * 2.0) / half)
    place = jnp.where(lane % half < freqs, position // GRID, position % GRID).astype(f32)
    angles = place * inverse
    sine = jnp.sin(angles)
    return jnp.cos(angles), jnp.where(lane % HEAD < half, -sine, sine)


def per_device(
    mixer_in,
    expert_in,
    mixer_gain,
    query_weight,
    key_weight,
    value_weight,
    query_gain,
    key_gain,
    output_weight,
    expert_gain,
    routes,
    route_weight,
    gate_weight,
    up_weight,
    down_weight,
):
    own = mixer_in.shape[0]
    owners, sides = lax.axis_size("ep"), lax.axis_size("tp") // 2
    ep = lax.axis_index("ep")
    offset = (ep * lax.axis_size("tp") + lax.axis_index("tp")) * own
    here = jnp.stack([ep >> 2, ep & 3]).astype(jnp.int32)
    cosine, sine = tables(offset, own)
    gain = mixer_gain.reshape(1, D)
    bound = (
        1.02 * HEAD**0.5 * jnp.max(jnp.abs(query_gain)) * jnp.max(jnp.abs(key_gain))
    ).reshape(1)

    def shifted(array, shift, back=False):
        down, across = divmod(shift, SIDE)
        pairs = []
        for z in range(SIDE):
            for x in range(SIDE):
                pair = (z * SIDE + x, (z + down) % SIDE * SIDE + (x + across) % SIDE)
                pairs.append(pair[::-1] if back else pair)
        return lax.ppermute(array, "ep", pairs)

    keyvals = pl.pallas_call(
        keyval_body,
        out_shape=jax.ShapeDtypeStruct((own, 2 * LANES), bf16),
        compiler_params=params(),
        cost_estimate=cost(own * D * 512, 2 * 2**20),
        name="keyval",
    )(mixer_in, gain, key_weight, value_weight, key_gain.reshape(1, HEAD), cosine, sine)
    line = jnp.concatenate(
        [keyvals] + [shifted(keyvals, SIDE * turn) for turn in range(1, SIDE)], axis=0
    )
    plane = jnp.concatenate([line] + [shifted(line, turn) for turn in range(1, SIDE)], axis=0)
    near = [plane]
    for turn in range(1, sides):
        ring = [(2 * y + c, 2 * ((y + turn) % sides) + c) for y in range(sides) for c in range(2)]
        near.append(lax.ppermute(plane, "tp", ring))
    near = jnp.concatenate(near, axis=0)
    far = lax.ppermute(near, "tp", [(i, i ^ 1) for i in range(2 * sides)])

    *first, normed, place, named = route(
        here,
        expert_in,
        expert_gain.reshape(1, D),
        routes.T,
        EXP_DEV * owners,
        GROUPS[0],
    )
    outgoing = dict(zip(GROUPS[0], first))
    rest = sum(GROUPS[1:], ())
    outgoing.update(zip(rest, dispatch(place, normed, rest)))
    queries = pl.pallas_call(
        query_body,
        out_shape=jax.ShapeDtypeStruct((QHEADS * own, 2 * LANES), bf16),
        compiler_params=params(),
        cost_estimate=cost(own * D * 2048, 5 * 2**20),
        name="query",
    )(mixer_in, gain, query_weight, query_gain.reshape(1, HEAD), cosine, sine)
    share = shares(place, named, route_weight.T)

    returned = {}
    for group in GROUPS:
        arrived = [
            shifted(array, shift) if shift else array
            for shift in group
            for array in (outgoing[shift],)
        ]
        results = expert(arrived, gate_weight, up_weight, down_weight)
        for shift, array in zip(group, results):
            returned[shift] = shifted(array, shift, True) if shift else array
    state = attend(bound, queries, near, None, own, False)
    attended = attend(bound, queries, far, state, own, True)
    mixer_out = jnp.dot(attended, output_weight, preferred_element_type=f32).astype(bf16)
    total = None
    for number, group in enumerate(GROUPS):
        arrays = [returned[shift] for shift in group]
        total = combine(share[number], arrays, total, number == len(GROUPS) - 1)
    return (mixer_out, total)


def solution(mesh):
    placed = (
        P(("ep", "tp"), None),
        P(("ep", "tp"), None),
        P(),
        P(),
        P(),
        P(),
        P(),
        P(),
        P(),
        P(),
        P(("ep", "tp"), None),
        P(("ep", "tp"), None),
        P("ep", None, None),
        P("ep", None, None),
        P("ep", None, None),
    )

    return jax.shard_map(
        per_device,
        mesh=mesh,
        in_specs=placed,
        out_specs=(P(("ep", "tp"), None), P(("ep", "tp"), None)),
        check_vma=False,
    )
```

```python
import functools

import jax
import jax.numpy as jnp
from jax import lax
from jax.experimental import pallas as pl
from jax.experimental.pallas import tpu as pltpu
from jax.sharding import PartitionSpec as P


D = 2048
HEAD = 64
QHEADS = 16
KVHEADS = 2
GRID = 64
FF = 512
TOPK = 2
EXP_DEV = 2
CAP = 64
LANES = 128
KEY_BLOCK = 2048
ROW_TILE = 512
SIDE = 4
GROUPS = ((0, 1, 3, 2, 4, 12, 8), (5, 15, 7, 13), (10, 6, 14, 9, 11))
BACK = (GROUPS[0] + GROUPS[1], GROUPS[2])
SAFE_LIMIT = 60.0
VMEM = 56 * 1024 * 1024

eps = 1e-06
theta = 10000.0
LOG2_E = 1.4426950408889634

f32 = jnp.float32
bf16 = jnp.bfloat16


def params(*semantics):
    return pltpu.CompilerParams(
        dimension_semantics=semantics or None, vmem_limit_bytes=VMEM
    )


def cost(flops, moved):
    return pl.CostEstimate(flops=int(flops), transcendentals=0, bytes_accessed=int(moved))


def normed_rows(values, gain):
    values = values.astype(f32)
    scaled = values * lax.rsqrt(jnp.mean(values * values, axis=-1, keepdims=True) + eps)
    return (scaled * gain).astype(bf16)


def head_pair(u, gain, cosine, sine):
    lane = lax.broadcasted_iota(jnp.int32, u.shape, 1)
    left = lane < HEAD
    square = u * u
    first = jnp.sum(jnp.where(left, square, 0.0), axis=-1, keepdims=True)
    second = jnp.sum(jnp.where(left, 0.0, square), axis=-1, keepdims=True)
    mean = jnp.where(left, first, second) * (1.0 / HEAD)
    u = u * lax.rsqrt(mean + eps) * gain
    half = HEAD // 2
    swapped = jnp.where(
        lane % HEAD < half, pltpu.roll(u, LANES - half, 1), pltpu.roll(u, half, 1)
    )
    return u * cosine + swapped * sine


def twice(gain):
    return jnp.concatenate([gain, gain], axis=1)


def keyval_body(x_ref, gain_ref, kw_ref, vw_ref, kgain_ref, cos_ref, sin_ref, out_ref):
    normed = normed_rows(x_ref[...], gain_ref[...])
    keys = jnp.dot(normed, kw_ref[...], preferred_element_type=f32)
    values = jnp.dot(normed, vw_ref[...], preferred_element_type=f32)
    out_ref[:, :LANES] = head_pair(keys, twice(kgain_ref[...]), cos_ref[...], sin_ref[...]).astype(bf16)
    out_ref[:, LANES:] = values.astype(bf16)


def query_body(x_ref, gain_ref, qw_ref, qgain_ref, cos_ref, sin_ref, out_ref):
    normed = normed_rows(x_ref[...], gain_ref[...])
    rows = x_ref.shape[0]
    left = lax.broadcasted_iota(jnp.int32, (rows, LANES), 1) < HEAD
    qgain = twice(qgain_ref[...])
    scale = HEAD ** (-0.5) * LOG2_E
    for pair in range(QHEADS // 2):
        u = jnp.dot(
            normed, qw_ref[:, pair * LANES : (pair + 1) * LANES], preferred_element_type=f32
        )
        u = head_pair(u, qgain, cos_ref[...], sin_ref[...])
        u = u.astype(bf16).astype(f32) * scale
        moved = pltpu.roll(u, HEAD, 1)
        for odd in range(2):
            head = 2 * pair + odd
            group = head // (QHEADS // KVHEADS)
            source = u if odd == group else moved
            keep = left if group == 0 else jnp.logical_not(left)
            source = jnp.where(keep, source, 0.0)
            high = source.astype(bf16)
            place = slice(head * rows, (head + 1) * rows)
            out_ref[place, :LANES] = high
            out_ref[place, LANES:] = (source - high.astype(f32)).astype(bf16)


def attend_body(safe_ref, q_ref, kv_ref, *refs, own, first, last):
    step = pl.program_id(0)
    if last:
        out_ref, peak_ref, acc_ref = refs[-3:]
    else:
        peak_ref, acc_ref = refs[-2:]

    @pl.when(step == 0)
    def _():
        if first:
            peak_ref[...] = jnp.full(peak_ref.shape, -jnp.inf, f32)
            acc_ref[...] = jnp.zeros(acc_ref.shape, f32)
        else:
            peak_ref[...] = refs[0][...]
            acc_ref[...] = refs[1][...]

    keys = kv_ref[:, :LANES]
    keys = jnp.concatenate([keys, keys], axis=1)
    values = kv_ref[:, LANES:]
    values = jnp.concatenate([values, jnp.ones(values.shape, bf16)], axis=1)

    def score(rows):
        return lax.dot_general(
            q_ref[rows, :], keys, (((1,), (1,)), ((), ())), preferred_element_type=f32
        )

    def gather(weights):
        return jnp.dot(weights.astype(bf16), values, preferred_element_type=f32)

    def plain(rows):
        acc_ref[rows, :] += gather(jnp.exp2(score(rows)))

    def careful(rows):
        scores = score(rows)
        before = peak_ref[rows, :1]
        fresh = jnp.maximum(before, jnp.max(scores, axis=-1, keepdims=True))
        peak_ref[rows, :] = jnp.broadcast_to(fresh, (fresh.shape[0], LANES))
        acc_ref[rows, :] = acc_ref[rows, :] * jnp.exp2(before - fresh) + gather(
            jnp.exp2(scores - fresh)
        )

    def sweep(work, tile, times):
        def some(index, carry):
            for time in range(times):
                start = pl.multiple_of((index * times + time) * tile, tile)
                work(pl.ds(start, tile))
            return carry

        lax.fori_loop(0, q_ref.shape[0] // (tile * times), some, 0)

    safe = safe_ref[0] <= SAFE_LIMIT

    @pl.when(safe)
    def _():
        sweep(plain, ROW_TILE, 2)

    @pl.when(jnp.logical_not(safe))
    def _():
        sweep(careful, ROW_TILE // 8, 1)

    if not last:
        return

    @pl.when(step == pl.num_programs(0) - 1)
    def _():
        left = lax.broadcasted_iota(jnp.int32, (own, LANES), 1) < HEAD
        for two in range(QHEADS // 2):
            done = []
            for head in (2 * two, 2 * two + 1):
                block = acc_ref[head * own : (head + 1) * own, :]
                done.append(block[:, :LANES] / block[:, LANES:])
            if 2 * two < QHEADS // KVHEADS:
                both = jnp.where(left, done[0], pltpu.roll(done[1], HEAD, 1))
            else:
                both = jnp.where(left, pltpu.roll(done[0], HEAD, 1), done[1])
            out_ref[:, two * LANES : (two + 1) * LANES] = both.astype(bf16)


def attend(safe, queries, keyvals, state, own, last):
    rows, keys = queries.shape[0], keyvals.shape[0]
    whole = lambda i: (0, 0)
    carried = [pl.BlockSpec((rows, LANES), whole), pl.BlockSpec((rows, 2 * LANES), whole)]
    shapes = [
        jax.ShapeDtypeStruct((rows, LANES), f32),
        jax.ShapeDtypeStruct((rows, 2 * LANES), f32),
    ]
    first = state is None
    return pl.pallas_call(
        functools.partial(attend_body, own=own, first=first, last=last),
        grid=(keys // KEY_BLOCK,),
        in_specs=[
            pl.BlockSpec(memory_space=pltpu.SMEM),
            pl.BlockSpec((rows, 2 * LANES), whole),
            pl.BlockSpec((KEY_BLOCK, 2 * LANES), lambda i: (i, 0)),
        ]
        + ([] if first else carried),
        out_specs=pl.BlockSpec((own, QHEADS * HEAD), whole) if last else carried,
        out_shape=jax.ShapeDtypeStruct((own, QHEADS * HEAD), bf16) if last else shapes,
        scratch_shapes=[pltpu.VMEM(shape.shape, f32) for shape in shapes] if last else [],
        compiler_params=params("arbitrary"),
        cost_estimate=cost(rows * keys * 1024, keys * 512),
        name="attend",
    )(safe, queries, keyvals, *([] if first else state))


def fill_pick(place_ref, pick_ref, group):
    slot = lax.broadcasted_iota(jnp.int32, (CAP, place_ref.shape[1]), 0).astype(f32)
    for index, shift in enumerate(group):
        for which in range(EXP_DEV):
            row = shift * EXP_DEV + which
            start = (index * EXP_DEV + which) * CAP
            pick_ref[start : start + CAP, :] = jnp.where(
                place_ref[row : row + 1, :] == slot, 1.0, 0.0
            ).astype(bf16)


def pick_rows(pick_ref, normed, out_refs):
    rows = jnp.dot(pick_ref[...], normed, preferred_element_type=f32).astype(bf16)
    span = EXP_DEV * CAP
    for index, out_ref in enumerate(out_refs):
        out_ref[...] = rows[index * span : (index + 1) * span].reshape(out_ref.shape)


def relative(routes, here_ref):
    holder = routes // EXP_DEV
    down = (holder // SIDE - here_ref[0] + SIDE) % SIDE
    across = (holder % SIDE - here_ref[1] + SIDE) % SIDE
    shift = down * here_ref[2] + across * here_ref[3]
    return shift * EXP_DEV + routes % EXP_DEV


def route_body(here_ref, x_ref, gain_ref, routes_ref, *refs, group):
    out_refs, (normed_ref, place_ref, named_ref, pick_ref) = refs[:-4], refs[-4:]
    step = pl.program_id(0)
    experts, tokens = place_ref.shape
    block = out_refs[0].shape[-1]

    @pl.when(step == 0)
    def _():
        named_ref[...] = relative(routes_ref[...], here_ref)
        expert = lax.broadcasted_iota(jnp.int32, (experts, tokens), 0)
        one = named_ref[0:1, :] == expert
        two = named_ref[1:2, :] == expert
        named = jnp.where(jnp.logical_or(one, two), 1.0, 0.0)
        row = lax.broadcasted_iota(jnp.int32, (tokens, tokens), 0)
        col = lax.broadcasted_iota(jnp.int32, (tokens, tokens), 1)
        earlier = jnp.where(row < col, 1.0, 0.0).astype(bf16)
        before = jnp.dot(named.astype(bf16), earlier, preferred_element_type=f32)
        place_ref[...] = jnp.where(named > 0.0, before, -1.0)
        fill_pick(place_ref, pick_ref, group)
        normed_ref[...] = normed_rows(x_ref[...], gain_ref[...])

    start = pl.multiple_of(step * block, block)
    pick_rows(pick_ref, normed_ref[:, pl.ds(start, block)], out_refs)


def bundles(count, block):
    return (
        [pl.BlockSpec((EXP_DEV, CAP, block), lambda i: (0, 0, i))] * count,
        [jax.ShapeDtypeStruct((EXP_DEV, CAP, D), bf16)] * count,
    )


def route(here, rows, gain, routes, experts, group):
    tokens = rows.shape[0]
    block = 512
    specs, shapes = bundles(len(group), block)
    whole = lambda i: (0, 0)
    return pl.pallas_call(
        functools.partial(route_body, group=group),
        grid=(D // block,),
        in_specs=[
            pl.BlockSpec(memory_space=pltpu.SMEM),
            pl.BlockSpec((tokens, D), whole),
            pl.BlockSpec((1, D), whole),
            pl.BlockSpec((TOPK, tokens), whole),
        ],
        out_specs=specs
        + [
            pl.BlockSpec((tokens, D), whole),
            pl.BlockSpec((experts, tokens), whole),
            pl.BlockSpec((TOPK, tokens), whole),
        ],
        out_shape=shapes
        + [
            jax.ShapeDtypeStruct((tokens, D), bf16),
            jax.ShapeDtypeStruct((experts, tokens), f32),
            jax.ShapeDtypeStruct((TOPK, tokens), jnp.int32),
        ],
        scratch_shapes=[pltpu.VMEM((len(group) * EXP_DEV * CAP, tokens), bf16)],
        compiler_params=params("arbitrary"),
        cost_estimate=cost(8e9, 8 * 2**20),
        name="route",
    )(here, rows, gain, routes)


def dispatch_body(place_ref, normed_ref, *refs, group):
    out_refs, pick_ref = refs[:-1], refs[-1]

    @pl.when(pl.program_id(0) == 0)
    def _():
        fill_pick(place_ref, pick_ref, group)

    pick_rows(pick_ref, normed_ref[...], out_refs)


def dispatch(place, normed, group):
    experts, tokens = place.shape
    block = 512
    specs, shapes = bundles(len(group), block)
    return pl.pallas_call(
        functools.partial(dispatch_body, group=group),
        grid=(D // block,),
        in_specs=[
            pl.BlockSpec((experts, tokens), lambda i: (0, 0)),
            pl.BlockSpec((tokens, block), lambda i: (0, i)),
        ],
        out_specs=specs,
        out_shape=shapes,
        scratch_shapes=[pltpu.VMEM((len(group) * EXP_DEV * CAP, tokens), bf16)],
        compiler_params=params("arbitrary"),
        cost_estimate=cost(5e9, 6 * 2**20),
        name="dispatch",
    )(place, normed)


def shares_body(place_ref, named_ref, weights_ref, *out_refs):
    experts, tokens = place_ref.shape
    expert = lax.broadcasted_iota(jnp.int32, (experts, tokens), 0)
    share = jnp.where(named_ref[0:1, :] == expert, weights_ref[0:1, :], 0.0) + jnp.where(
        named_ref[1:2, :] == expert, weights_ref[1:2, :], 0.0
    )
    slot = lax.broadcasted_iota(jnp.int32, (CAP, tokens), 0).astype(f32)
    for group, out_ref in zip(BACK, out_refs):
        for index, shift in enumerate(group):
            tiles = []
            for which in range(EXP_DEV):
                row = slice(shift * EXP_DEV + which, shift * EXP_DEV + which + 1)
                tiles.append(jnp.where(place_ref[row, :] == slot, share[row, :], 0.0))
            value = jnp.concatenate(tiles, axis=0).T
            high = value.astype(bf16)
            low = (value - high.astype(f32)).astype(bf16)
            columns = slice(index * LANES, (index + 1) * LANES)
            out_ref[:tokens, columns] = high
            out_ref[tokens:, columns] = low


def shares(place, named, weights):
    tokens = place.shape[1]
    return pl.pallas_call(
        shares_body,
        out_shape=[
            jax.ShapeDtypeStruct((2 * tokens, len(group) * LANES), bf16) for group in BACK
        ],
        compiler_params=params(),
        cost_estimate=cost(4e9, 4 * 2**20),
        name="shares",
    )(place, named, weights)


def expert_body(gate_ref, up_ref, down_ref, *refs):
    count = len(refs) // 2
    rows = jnp.concatenate([ref[0] for ref in refs[:count]], axis=0)
    gate = jnp.dot(rows, gate_ref[0], preferred_element_type=f32)
    upper = jnp.dot(rows, up_ref[0], preferred_element_type=f32)
    hidden = (gate * (1.0 / (1.0 + jnp.exp(-gate))) * upper).astype(bf16)
    result = jnp.dot(hidden, down_ref[0], preferred_element_type=f32).astype(bf16)
    for index, out_ref in enumerate(refs[count:]):
        out_ref[0] = result[index * CAP : (index + 1) * CAP]


def expert(arrays, gate, up, down):
    each = lambda i: (i, 0, 0)
    count = len(arrays)
    rows = [pl.BlockSpec((1, CAP, D), each)] * count
    return pl.pallas_call(
        expert_body,
        grid=(EXP_DEV,),
        in_specs=[
            pl.BlockSpec((1, D, FF), each),
            pl.BlockSpec((1, D, FF), each),
            pl.BlockSpec((1, FF, D), each),
        ]
        + rows,
        out_specs=rows,
        out_shape=[jax.ShapeDtypeStruct((EXP_DEV, CAP, D), bf16)] * count,
        compiler_params=params("arbitrary"),
        cost_estimate=cost(6 * count * EXP_DEV * CAP * D * FF, 14 * 2**20),
        name="expert",
    )(gate, up, down, *arrays)


def combine_body(share_ref, *refs, first):
    out_ref = refs[-1]
    back_refs = refs[:-1] if first else refs[:-2]
    tokens = out_ref.shape[0]
    back = jnp.concatenate([ref[...].reshape(-1, ref.shape[-1]) for ref in back_refs], axis=0)
    both = jnp.dot(share_ref[...], back, preferred_element_type=f32)
    total = both[:tokens] + both[tokens:]
    if not first:
        total = total + refs[-2][...]
    out_ref[...] = total.astype(out_ref.dtype)


def combine(share, arrays, part, last):
    tokens = share.shape[0] // 2
    block = 512
    column = pl.BlockSpec((tokens, block), lambda i: (0, i))
    specs = [pl.BlockSpec(share.shape, lambda i: (0, 0))] + bundles(len(arrays), block)[0]
    operands = [share, *arrays]
    if part is not None:
        specs.append(column)
        operands.append(part)
    return pl.pallas_call(
        functools.partial(combine_body, first=part is None),
        grid=(D // block,),
        in_specs=specs,
        out_specs=column,
        out_shape=jax.ShapeDtypeStruct((tokens, D), bf16 if last else f32),
        compiler_params=params("arbitrary"),
        cost_estimate=cost(4 * share.shape[1] * tokens * D, 8 * 2**20),
        name="combine",
    )(*operands)


def tables(offset, count):
    lane = jnp.arange(LANES, dtype=jnp.int32)[None, :] + jnp.zeros((count, 1), jnp.int32)
    position = offset + jnp.arange(count, dtype=jnp.int32)[:, None] + jnp.zeros_like(lane)
    half = HEAD // 2
    freqs = half // 2
    inverse = theta ** (-((lane % freqs).astype(f32) * 2.0) / half)
    place = jnp.where(lane % half < freqs, position // GRID, position % GRID).astype(f32)
    angles = place * inverse
    sine = jnp.sin(angles)
    return jnp.cos(angles), jnp.where(lane % HEAD < half, -sine, sine)


def per_device(
    mixer_in,
    expert_in,
    mixer_gain,
    query_weight,
    key_weight,
    value_weight,
    query_gain,
    key_gain,
    output_weight,
    expert_gain,
    routes,
    route_weight,
    gate_weight,
    up_weight,
    down_weight,
):
    own = mixer_in.shape[0]
    owners, sides = lax.axis_size("ep"), lax.axis_size("tp") // 2
    ep = lax.axis_index("ep")
    offset = (ep * lax.axis_size("tp") + lax.axis_index("tp")) * own
    core = lax.axis_index("tp") & 1
    here = jnp.stack([ep >> 2, ep & 3, SIDE - 3 * core, 1 + 3 * core]).astype(jnp.int32)
    cosine, sine = tables(offset, own)
    gain = mixer_gain.reshape(1, D)
    bound = (
        1.02 * HEAD**0.5 * jnp.max(jnp.abs(query_gain)) * jnp.max(jnp.abs(key_gain))
    ).reshape(1)

    def shifted(array, shift, back=False):
        pairs = []
        for source in range(owners * 2 * sides):
            holder, member = divmod(source, 2 * sides)
            turns = divmod(shift, SIDE)
            down, across = turns[::-1] if member & 1 else turns
            z, x = divmod(holder, SIDE)
            target = (z + down) % SIDE * SIDE + (x + across) % SIDE
            pair = (source, target * 2 * sides + member)
            pairs.append(pair[::-1] if back else pair)
        return lax.ppermute(array, ("ep", "tp"), pairs)

    keyvals = pl.pallas_call(
        keyval_body,
        out_shape=jax.ShapeDtypeStruct((own, 2 * LANES), bf16),
        compiler_params=params(),
        cost_estimate=cost(own * D * 512, 2 * 2**20),
        name="keyval",
    )(mixer_in, gain, key_weight, value_weight, key_gain.reshape(1, HEAD), cosine, sine)
    line = jnp.concatenate(
        [keyvals] + [shifted(keyvals, SIDE * turn) for turn in range(1, SIDE)], axis=0
    )
    plane = jnp.concatenate([line] + [shifted(line, turn) for turn in range(1, SIDE)], axis=0)
    near = [plane]
    for turn in range(1, sides):
        ring = [(2 * y + c, 2 * ((y + turn) % sides) + c) for y in range(sides) for c in range(2)]
        near.append(lax.ppermute(plane, "tp", ring))
    near = jnp.concatenate(near, axis=0)
    far = lax.ppermute(near, "tp", [(i, i ^ 1) for i in range(2 * sides)])

    *first, normed, place, named = route(
        here,
        expert_in,
        expert_gain.reshape(1, D),
        routes.T,
        EXP_DEV * owners,
        GROUPS[0],
    )
    outgoing = dict(zip(GROUPS[0], first))
    rest = sum(GROUPS[1:], ())
    outgoing.update(zip(rest, dispatch(place, normed, rest)))
    queries = pl.pallas_call(
        query_body,
        out_shape=jax.ShapeDtypeStruct((QHEADS * own, 2 * LANES), bf16),
        compiler_params=params(),
        cost_estimate=cost(own * D * 2048, 5 * 2**20),
        name="query",
    )(mixer_in, gain, query_weight, query_gain.reshape(1, HEAD), cosine, sine)
    share = shares(place, named, route_weight.T)

    returned = {}
    for group in GROUPS:
        arrived = [
            shifted(array, shift) if shift else array
            for shift in group
            for array in (outgoing[shift],)
        ]
        results = expert(arrived, gate_weight, up_weight, down_weight)
        for shift, array in zip(group, results):
            returned[shift] = shifted(array, shift, True) if shift else array
    state = attend(bound, queries, near, None, own, False)
    attended = attend(bound, queries, far, state, own, True)
    mixer_out = jnp.dot(attended, output_weight, preferred_element_type=f32).astype(bf16)
    total = None
    for number, group in enumerate(BACK):
        arrays = [returned[shift] for shift in group]
        total = combine(share[number], arrays, total, number == len(BACK) - 1)
    return (mixer_out, total)


def solution(mesh):
    placed = (
        P(("ep", "tp"), None),
        P(("ep", "tp"), None),
        P(),
        P(),
        P(),
        P(),
        P(),
        P(),
        P(),
        P(),
        P(("ep", "tp"), None),
        P(("ep", "tp"), None),
        P("ep", None, None),
        P("ep", None, None),
        P("ep", None, None),
    )

    return jax.shard_map(
        per_device,
        mesh=mesh,
        in_specs=placed,
        out_specs=(P(("ep", "tp"), None), P(("ep", "tp"), None)),
        check_vma=False,
    )
```

```python
import functools

import jax
import jax.numpy as jnp
from jax import lax
from jax.experimental import pallas as pl
from jax.experimental.pallas import tpu as pltpu
from jax.sharding import PartitionSpec as P


D = 2048
HEAD = 64
QHEADS = 16
KVHEADS = 2
GRID = 64
FF = 512
TOPK = 2
EXP_DEV = 2
CAP = 64
LANES = 128
KEY_BLOCK = 2048
ROW_TILE = 512
SIDE = 4
GROUPS = ((0, 1, 3, 4, 12), (2, 8, 5, 15, 7, 13), (10, 6, 14, 9, 11))
BACK = (GROUPS[0] + GROUPS[1], GROUPS[2])
SAFE_LIMIT = 60.0
VMEM = 56 * 1024 * 1024

eps = 1e-06
theta = 10000.0
LOG2_E = 1.4426950408889634

f32 = jnp.float32
bf16 = jnp.bfloat16


def params(*semantics):
    return pltpu.CompilerParams(
        dimension_semantics=semantics or None, vmem_limit_bytes=VMEM
    )


def cost(flops, moved):
    return pl.CostEstimate(flops=int(flops), transcendentals=0, bytes_accessed=int(moved))


def normed_rows(values, gain):
    values = values.astype(f32)
    scaled = values * lax.rsqrt(jnp.mean(values * values, axis=-1, keepdims=True) + eps)
    return (scaled * gain).astype(bf16)


def head_pair(u, gain, cosine, sine):
    lane = lax.broadcasted_iota(jnp.int32, u.shape, 1)
    left = lane < HEAD
    square = u * u
    first = jnp.sum(jnp.where(left, square, 0.0), axis=-1, keepdims=True)
    second = jnp.sum(jnp.where(left, 0.0, square), axis=-1, keepdims=True)
    mean = jnp.where(left, first, second) * (1.0 / HEAD)
    u = u * lax.rsqrt(mean + eps) * gain
    half = HEAD // 2
    swapped = jnp.where(
        lane % HEAD < half, pltpu.roll(u, LANES - half, 1), pltpu.roll(u, half, 1)
    )
    return u * cosine + swapped * sine


def twice(gain):
    return jnp.concatenate([gain, gain], axis=1)


def keyval_body(x_ref, gain_ref, kw_ref, vw_ref, kgain_ref, cos_ref, sin_ref, out_ref):
    normed = normed_rows(x_ref[...], gain_ref[...])
    keys = jnp.dot(normed, kw_ref[...], preferred_element_type=f32)
    values = jnp.dot(normed, vw_ref[...], preferred_element_type=f32)
    keys = head_pair(keys, twice(kgain_ref[...]), cos_ref[...], sin_ref[...]).astype(bf16)
    both = jnp.concatenate([keys, values.astype(bf16)], axis=1)
    for index in range(out_ref.shape[0]):
        out_ref[index] = both


def query_body(x_ref, gain_ref, qw_ref, qgain_ref, cos_ref, sin_ref, out_ref):
    normed = normed_rows(x_ref[...], gain_ref[...])
    rows = x_ref.shape[0]
    left = lax.broadcasted_iota(jnp.int32, (rows, LANES), 1) < HEAD
    qgain = twice(qgain_ref[...])
    scale = HEAD ** (-0.5) * LOG2_E
    for pair in range(QHEADS // 2):
        u = jnp.dot(
            normed, qw_ref[:, pair * LANES : (pair + 1) * LANES], preferred_element_type=f32
        )
        u = head_pair(u, qgain, cos_ref[...], sin_ref[...])
        u = u.astype(bf16).astype(f32) * scale
        moved = pltpu.roll(u, HEAD, 1)
        for odd in range(2):
            head = 2 * pair + odd
            group = head // (QHEADS // KVHEADS)
            source = u if odd == group else moved
            keep = left if group == 0 else jnp.logical_not(left)
            source = jnp.where(keep, source, 0.0)
            high = source.astype(bf16)
            place = slice(head * rows, (head + 1) * rows)
            out_ref[place, :LANES] = high
            out_ref[place, LANES:] = (source - high.astype(f32)).astype(bf16)


def attend_body(safe_ref, q_ref, kv_ref, *refs, own, first, last):
    step = pl.program_id(0)
    if last:
        out_ref, peak_ref, acc_ref = refs[-3:]
    else:
        peak_ref, acc_ref = refs[-2:]

    @pl.when(step == 0)
    def _():
        if first:
            peak_ref[...] = jnp.full(peak_ref.shape, -jnp.inf, f32)
            acc_ref[...] = jnp.zeros(acc_ref.shape, f32)
        else:
            peak_ref[...] = refs[0][...]
            acc_ref[...] = refs[1][...]

    keys = kv_ref[:, :LANES]
    keys = jnp.concatenate([keys, keys], axis=1)
    values = kv_ref[:, LANES:]
    values = jnp.concatenate([values, jnp.ones(values.shape, bf16)], axis=1)

    def score(rows):
        return lax.dot_general(
            q_ref[rows, :], keys, (((1,), (1,)), ((), ())), preferred_element_type=f32
        )

    def gather(weights):
        return jnp.dot(weights.astype(bf16), values, preferred_element_type=f32)

    def plain(rows):
        acc_ref[rows, :] += gather(jnp.exp2(score(rows)))

    def careful(rows):
        scores = score(rows)
        before = peak_ref[rows, :1]
        fresh = jnp.maximum(before, jnp.max(scores, axis=-1, keepdims=True))
        peak_ref[rows, :] = jnp.broadcast_to(fresh, (fresh.shape[0], LANES))
        acc_ref[rows, :] = acc_ref[rows, :] * jnp.exp2(before - fresh) + gather(
            jnp.exp2(scores - fresh)
        )

    def sweep(work, tile, times):
        def some(index, carry):
            for time in range(times):
                start = pl.multiple_of((index * times + time) * tile, tile)
                work(pl.ds(start, tile))
            return carry

        lax.fori_loop(0, q_ref.shape[0] // (tile * times), some, 0)

    safe = safe_ref[0] <= SAFE_LIMIT

    @pl.when(safe)
    def _():
        sweep(plain, ROW_TILE, 2)

    @pl.when(jnp.logical_not(safe))
    def _():
        sweep(careful, ROW_TILE // 8, 1)

    if not last:
        return

    @pl.when(step == pl.num_programs(0) - 1)
    def _():
        left = lax.broadcasted_iota(jnp.int32, (own, LANES), 1) < HEAD
        for two in range(QHEADS // 2):
            done = []
            for head in (2 * two, 2 * two + 1):
                block = acc_ref[head * own : (head + 1) * own, :]
                done.append(block[:, :LANES] / block[:, LANES:])
            if 2 * two < QHEADS // KVHEADS:
                both = jnp.where(left, done[0], pltpu.roll(done[1], HEAD, 1))
            else:
                both = jnp.where(left, pltpu.roll(done[0], HEAD, 1), done[1])
            out_ref[:, two * LANES : (two + 1) * LANES] = both.astype(bf16)


def attend(safe, queries, keyvals, state, own, last):
    rows, keys = queries.shape[0], keyvals.shape[0]
    whole = lambda i: (0, 0)
    carried = [pl.BlockSpec((rows, LANES), whole), pl.BlockSpec((rows, 2 * LANES), whole)]
    shapes = [
        jax.ShapeDtypeStruct((rows, LANES), f32),
        jax.ShapeDtypeStruct((rows, 2 * LANES), f32),
    ]
    first = state is None
    return pl.pallas_call(
        functools.partial(attend_body, own=own, first=first, last=last),
        grid=(keys // KEY_BLOCK,),
        in_specs=[
            pl.BlockSpec(memory_space=pltpu.SMEM),
            pl.BlockSpec((rows, 2 * LANES), whole),
            pl.BlockSpec((KEY_BLOCK, 2 * LANES), lambda i: (i, 0)),
        ]
        + ([] if first else carried),
        out_specs=pl.BlockSpec((own, QHEADS * HEAD), whole) if last else carried,
        out_shape=jax.ShapeDtypeStruct((own, QHEADS * HEAD), bf16) if last else shapes,
        scratch_shapes=[pltpu.VMEM(shape.shape, f32) for shape in shapes] if last else [],
        compiler_params=params("arbitrary"),
        cost_estimate=cost(rows * keys * 1024, keys * 512),
        name="attend",
    )(safe, queries, keyvals, *([] if first else state))


def fill_pick(place_ref, pick_ref, group):
    slot = lax.broadcasted_iota(jnp.int32, (CAP, place_ref.shape[1]), 0).astype(f32)
    for index, shift in enumerate(group):
        for which in range(EXP_DEV):
            row = shift * EXP_DEV + which
            start = (index * EXP_DEV + which) * CAP
            pick_ref[start : start + CAP, :] = jnp.where(
                place_ref[row : row + 1, :] == slot, 1.0, 0.0
            ).astype(bf16)


def pick_rows(pick_ref, normed, out_refs):
    rows = jnp.dot(pick_ref[...], normed, preferred_element_type=f32).astype(bf16)
    span = EXP_DEV * CAP
    for index, out_ref in enumerate(out_refs):
        out_ref[...] = rows[index * span : (index + 1) * span].reshape(out_ref.shape)


def relative(routes, here_ref):
    holder = routes // EXP_DEV
    down = (holder // SIDE - here_ref[0] + SIDE) % SIDE
    across = (holder % SIDE - here_ref[1] + SIDE) % SIDE
    shift = down * here_ref[2] + across * here_ref[3]
    return shift * EXP_DEV + routes % EXP_DEV


def route_body(here_ref, x_ref, gain_ref, routes_ref, *refs, group):
    out_refs, (normed_ref, place_ref, named_ref, pick_ref) = refs[:-4], refs[-4:]
    step = pl.program_id(0)
    experts, tokens = place_ref.shape
    block = out_refs[0].shape[-1]

    @pl.when(step == 0)
    def _():
        named_ref[...] = relative(routes_ref[...], here_ref)
        expert = lax.broadcasted_iota(jnp.int32, (experts, tokens), 0)
        one = named_ref[0:1, :] == expert
        two = named_ref[1:2, :] == expert
        named = jnp.where(jnp.logical_or(one, two), 1.0, 0.0)
        row = lax.broadcasted_iota(jnp.int32, (tokens, tokens), 0)
        col = lax.broadcasted_iota(jnp.int32, (tokens, tokens), 1)
        earlier = jnp.where(row < col, 1.0, 0.0).astype(bf16)
        before = jnp.dot(named.astype(bf16), earlier, preferred_element_type=f32)
        place_ref[...] = jnp.where(named > 0.0, before, -1.0)
        fill_pick(place_ref, pick_ref, group)
        normed_ref[...] = normed_rows(x_ref[...], gain_ref[...])

    start = pl.multiple_of(step * block, block)
    pick_rows(pick_ref, normed_ref[:, pl.ds(start, block)], out_refs)


def bundles(count, block):
    return (
        [pl.BlockSpec((EXP_DEV, CAP, block), lambda i: (0, 0, i))] * count,
        [jax.ShapeDtypeStruct((EXP_DEV, CAP, D), bf16)] * count,
    )


def route(here, rows, gain, routes, experts, group):
    tokens = rows.shape[0]
    block = 512
    specs, shapes = bundles(len(group), block)
    whole = lambda i: (0, 0)
    return pl.pallas_call(
        functools.partial(route_body, group=group),
        grid=(D // block,),
        in_specs=[
            pl.BlockSpec(memory_space=pltpu.SMEM),
            pl.BlockSpec((tokens, D), whole),
            pl.BlockSpec((1, D), whole),
            pl.BlockSpec((TOPK, tokens), whole),
        ],
        out_specs=specs
        + [
            pl.BlockSpec((tokens, D), whole),
            pl.BlockSpec((experts, tokens), whole),
            pl.BlockSpec((TOPK, tokens), whole),
        ],
        out_shape=shapes
        + [
            jax.ShapeDtypeStruct((tokens, D), bf16),
            jax.ShapeDtypeStruct((experts, tokens), f32),
            jax.ShapeDtypeStruct((TOPK, tokens), jnp.int32),
        ],
        scratch_shapes=[pltpu.VMEM((len(group) * EXP_DEV * CAP, tokens), bf16)],
        compiler_params=params("arbitrary"),
        cost_estimate=cost(8e9, 8 * 2**20),
        name="route",
    )(here, rows, gain, routes)


def dispatch_body(place_ref, normed_ref, *refs, group):
    out_refs, pick_ref = refs[:-1], refs[-1]

    @pl.when(pl.program_id(0) == 0)
    def _():
        fill_pick(place_ref, pick_ref, group)

    pick_rows(pick_ref, normed_ref[...], out_refs)


def dispatch(place, normed, group):
    experts, tokens = place.shape
    block = 512
    specs, shapes = bundles(len(group), block)
    return pl.pallas_call(
        functools.partial(dispatch_body, group=group),
        grid=(D // block,),
        in_specs=[
            pl.BlockSpec((experts, tokens), lambda i: (0, 0)),
            pl.BlockSpec((tokens, block), lambda i: (0, i)),
        ],
        out_specs=specs,
        out_shape=shapes,
        scratch_shapes=[pltpu.VMEM((len(group) * EXP_DEV * CAP, tokens), bf16)],
        compiler_params=params("arbitrary"),
        cost_estimate=cost(5e9, 6 * 2**20),
        name="dispatch",
    )(place, normed)


def shares_body(place_ref, named_ref, weights_ref, *out_refs):
    experts, tokens = place_ref.shape
    expert = lax.broadcasted_iota(jnp.int32, (experts, tokens), 0)
    share = jnp.where(named_ref[0:1, :] == expert, weights_ref[0:1, :], 0.0) + jnp.where(
        named_ref[1:2, :] == expert, weights_ref[1:2, :], 0.0
    )
    slot = lax.broadcasted_iota(jnp.int32, (CAP, tokens), 0).astype(f32)
    for group, out_ref in zip(BACK, out_refs):
        for index, shift in enumerate(group):
            tiles = []
            for which in range(EXP_DEV):
                row = slice(shift * EXP_DEV + which, shift * EXP_DEV + which + 1)
                tiles.append(jnp.where(place_ref[row, :] == slot, share[row, :], 0.0))
            columns = slice(index * LANES, (index + 1) * LANES)
            out_ref[:, columns] = jnp.concatenate(tiles, axis=0).T.astype(bf16)


def shares(place, named, weights):
    tokens = place.shape[1]
    return pl.pallas_call(
        shares_body,
        out_shape=[
            jax.ShapeDtypeStruct((tokens, len(group) * LANES), bf16) for group in BACK
        ],
        compiler_params=params(),
        cost_estimate=cost(4e9, 4 * 2**20),
        name="shares",
    )(place, named, weights)


def expert_body(gate_ref, up_ref, down_ref, *refs):
    count = len(refs) // 2
    rows = jnp.concatenate([ref[0] for ref in refs[:count]], axis=0)
    gate = jnp.dot(rows, gate_ref[0], preferred_element_type=f32)
    upper = jnp.dot(rows, up_ref[0], preferred_element_type=f32)
    hidden = (gate * (1.0 / (1.0 + jnp.exp(-gate))) * upper).astype(bf16)
    result = jnp.dot(hidden, down_ref[0], preferred_element_type=f32).astype(bf16)
    for index, out_ref in enumerate(refs[count:]):
        out_ref[0] = result[index * CAP : (index + 1) * CAP]


def expert(arrays, gate, up, down):
    each = lambda i: (i, 0, 0)
    count = len(arrays)
    rows = [pl.BlockSpec((1, CAP, D), each)] * count
    return pl.pallas_call(
        expert_body,
        grid=(EXP_DEV,),
        in_specs=[
            pl.BlockSpec((1, D, FF), each),
            pl.BlockSpec((1, D, FF), each),
            pl.BlockSpec((1, FF, D), each),
        ]
        + rows,
        out_specs=rows,
        out_shape=[jax.ShapeDtypeStruct((EXP_DEV, CAP, D), bf16)] * count,
        compiler_params=params("arbitrary"),
        cost_estimate=cost(6 * count * EXP_DEV * CAP * D * FF, 14 * 2**20),
        name="expert",
    )(gate, up, down, *arrays)


def combine_body(share_ref, *refs, first):
    out_ref = refs[-1]
    back_refs = refs[:-1] if first else refs[:-2]
    back = jnp.concatenate([ref[...].reshape(-1, ref.shape[-1]) for ref in back_refs], axis=0)
    total = jnp.dot(share_ref[...], back, preferred_element_type=f32)
    if not first:
        total = total + refs[-2][...]
    out_ref[...] = total.astype(out_ref.dtype)


def combine(share, arrays, part, last):
    tokens = share.shape[0]
    block = 512
    column = pl.BlockSpec((tokens, block), lambda i: (0, i))
    specs = [pl.BlockSpec(share.shape, lambda i: (0, 0))] + bundles(len(arrays), block)[0]
    operands = [share, *arrays]
    if part is not None:
        specs.append(column)
        operands.append(part)
    return pl.pallas_call(
        functools.partial(combine_body, first=part is None),
        grid=(D // block,),
        in_specs=specs,
        out_specs=column,
        out_shape=jax.ShapeDtypeStruct((tokens, D), bf16 if last else f32),
        compiler_params=params("arbitrary"),
        cost_estimate=cost(4 * share.shape[1] * tokens * D, 8 * 2**20),
        name="combine",
    )(*operands)


def tables(offset, count):
    lane = jnp.arange(LANES, dtype=jnp.int32)[None, :] + jnp.zeros((count, 1), jnp.int32)
    position = offset + jnp.arange(count, dtype=jnp.int32)[:, None] + jnp.zeros_like(lane)
    half = HEAD // 2
    freqs = half // 2
    inverse = theta ** (-((lane % freqs).astype(f32) * 2.0) / half)
    place = jnp.where(lane % half < freqs, position // GRID, position % GRID).astype(f32)
    angles = place * inverse
    sine = jnp.sin(angles)
    return jnp.cos(angles), jnp.where(lane % HEAD < half, -sine, sine)


def per_device(
    mixer_in,
    expert_in,
    mixer_gain,
    query_weight,
    key_weight,
    value_weight,
    query_gain,
    key_gain,
    output_weight,
    expert_gain,
    routes,
    route_weight,
    gate_weight,
    up_weight,
    down_weight,
):
    own = mixer_in.shape[0]
    owners, sides = lax.axis_size("ep"), lax.axis_size("tp") // 2
    ep = lax.axis_index("ep")
    offset = (ep * lax.axis_size("tp") + lax.axis_index("tp")) * own
    core = lax.axis_index("tp") & 1
    here = jnp.stack([ep >> 2, ep & 3, SIDE - 3 * core, 1 + 3 * core]).astype(jnp.int32)
    cosine, sine = tables(offset, own)
    gain = mixer_gain.reshape(1, D)
    bound = (
        1.02 * HEAD**0.5 * jnp.max(jnp.abs(query_gain)) * jnp.max(jnp.abs(key_gain))
    ).reshape(1)

    def shifted(array, shift, back=False):
        pairs = []
        for source in range(owners * 2 * sides):
            holder, member = divmod(source, 2 * sides)
            turns = divmod(shift, SIDE)
            down, across = turns[::-1] if member & 1 else turns
            z, x = divmod(holder, SIDE)
            target = (z + down) % SIDE * SIDE + (x + across) % SIDE
            pair = (source, target * 2 * sides + member)
            pairs.append(pair[::-1] if back else pair)
        return lax.ppermute(array, ("ep", "tp"), pairs)

    keyvals = pl.pallas_call(
        keyval_body,
        out_shape=jax.ShapeDtypeStruct((owners, own, 2 * LANES), bf16),
        compiler_params=params(),
        cost_estimate=cost(own * D * 512, 2 * 2**20),
        name="keyval",
    )(mixer_in, gain, key_weight, value_weight, key_gain.reshape(1, HEAD), cosine, sine)
    plane = lax.all_to_all(keyvals, "ep", split_axis=0, concat_axis=0, tiled=True)
    plane = plane.reshape(owners * own, 2 * LANES)
    near = [plane]
    for turn in range(1, sides):
        ring = [(2 * y + c, 2 * ((y + turn) % sides) + c) for y in range(sides) for c in range(2)]
        near.append(lax.ppermute(plane, "tp", ring))
    near = jnp.concatenate(near, axis=0)
    far = lax.ppermute(near, "tp", [(i, i ^ 1) for i in range(2 * sides)])

    *first, normed, place, named = route(
        here,
        expert_in,
        expert_gain.reshape(1, D),
        routes.T,
        EXP_DEV * owners,
        GROUPS[0],
    )
    outgoing = dict(zip(GROUPS[0], first))
    rest = sum(GROUPS[1:], ())
    outgoing.update(zip(rest, dispatch(place, normed, rest)))
    queries = pl.pallas_call(
        query_body,
        out_shape=jax.ShapeDtypeStruct((QHEADS * own, 2 * LANES), bf16),
        compiler_params=params(),
        cost_estimate=cost(own * D * 2048, 5 * 2**20),
        name="query",
    )(mixer_in, gain, query_weight, query_gain.reshape(1, HEAD), cosine, sine)
    share = shares(place, named, route_weight.T)

    returned = {}
    for group in GROUPS:
        arrived = [
            shifted(array, shift) if shift else array
            for shift in group
            for array in (outgoing[shift],)
        ]
        results = expert(arrived, gate_weight, up_weight, down_weight)
        for shift, array in zip(group, results):
            returned[shift] = shifted(array, shift, True) if shift else array
    state = attend(bound, queries, near, None, own, False)
    attended = attend(bound, queries, far, state, own, True)
    mixer_out = jnp.dot(attended, output_weight, preferred_element_type=f32).astype(bf16)
    total = None
    for number, group in enumerate(BACK):
        arrays = [returned[shift] for shift in group]
        total = combine(share[number], arrays, total, number == len(BACK) - 1)
    return (mixer_out, total)


def solution(mesh):
    placed = (
        P(("ep", "tp"), None),
        P(("ep", "tp"), None),
        P(),
        P(),
        P(),
        P(),
        P(),
        P(),
        P(),
        P(),
        P(("ep", "tp"), None),
        P(("ep", "tp"), None),
        P("ep", None, None),
        P("ep", None, None),
        P("ep", None, None),
    )

    return jax.shard_map(
        per_device,
        mesh=mesh,
        in_specs=placed,
        out_specs=(P(("ep", "tp"), None), P(("ep", "tp"), None)),
        check_vma=False,
    )
```
